32 devices in a mesh: grp: 2 (over y), sp: 4 (over z), tp: 4 (over x, core).
Axes of the slice: x: 2, y: 2, z: 4, core: 2. Of those that a mesh axis runs over, the one named last changes fastest.
Arguments:
- latent: bfloat16 [4096, 4096], P(('grp', 'sp', 'tp')), parts along dimension 0, may hold values from -260 to 260
- context: bfloat16 [1536, 4096], P(('grp', 'sp')), parts along dimension 0, may hold values from -6 to 6
- conditioning: bfloat16 [8192], P(('grp', 'sp')), parts along dimension 0, may hold values from -6 to 6
- norm_gain: float32 [4096], replicated, may hold values from 0.1 to 1.9
- shift_weight: bfloat16 [4096, 4096], P('sp', 'tp'), may hold values from -0.09375 to 0.09375
- scale_weight: bfloat16 [4096, 4096], P('sp', 'tp'), may hold values from -0.09375 to 0.09375
- gate_weight: bfloat16 [4096, 4096], P('sp', 'tp'), may hold values from -0.09375 to 0.09375
- query_weight: bfloat16 [4096, 1024], P(None, 'tp'), may hold values from -3 to 3
- key_weight: bfloat16 [4096, 512], P(None, 'tp'), may hold values from -3 to 3
- value_weight: bfloat16 [4096, 512], P(None, 'tp'), may hold values from -0.09375 to 0.09375
- out_weight: bfloat16 [1024, 4096], P(None, 'tp'), may hold values from -1.5 to 1.5
- sink_logit: float32 [16], P('tp'), may hold values from 3 to 7
Outputs:
- mixed: bfloat16 [4096, 4096], P(('grp', 'sp', 'tp')), parts along dimension 0
The draws below stay inside these ranges and needn't reach their ends.
There are 2 independent parts, one for each index of `grp`. The reference program is written for one: setup_inputs(seed, part) draws one part's arguments, and reference() takes and returns one part's arrays. A program takes and returns all parts, laid end to end along the dimension named above; an argument that names none is the same for every part. Nothing has to cross between parts.
All inputs are finite; a program needn't handle non-finite values.
Results may differ from the reference program's by a relative error of at most 0.012.
The reference program's roundings to bfloat16 on the way count: a program that leaves them out, or rounds other values in their place, can miss the bound.
Values may be sent and summed in bfloat16 or wider, within the bound.
No kernel may reach another device: no remote copies, remote signals or barrier semaphores. Data moves between devices by JAX's collectives and lax.ppermute only.
A program may use at most 64 MiB of HBM per device.

```python
import math
import jax
import jax.numpy as jnp
from jax import lax

D = 4096
HEADS = 16
KV_HEADS = 8
HD = 64
GRID_W = 64
WIN = 128
CTX = 768
SEQ = 2048


def paired_projections(seed_key):
    query_rows = jax.random.truncated_normal(jax.random.fold_in(seed_key, 11), -4.0, 4.0, (D, HEADS * HD), jnp.float32) / math.sqrt(D)
    key_rows = jax.random.truncated_normal(jax.random.fold_in(seed_key, 12), -4.0, 4.0, (D, KV_HEADS * HD), jnp.float32) / math.sqrt(D)
    return (query_rows, key_rows)


def draw_query_weight(key, part):
    return paired_projections(key)[0].astype(jnp.bfloat16)


def draw_key_weight(key, part):
    return paired_projections(key)[1].astype(jnp.bfloat16)


def draw_latent(key, part):
    values_drawn = jax.random.truncated_normal(jax.random.fold_in(key, 1), -6.0, 6.0, (SEQ, D), jnp.float32)
    return values_drawn.astype(jnp.bfloat16)


def block_scale(rng, extent, cuts, least, high):
    factor_of, own = 1.0, jax.random.fold_in(rng, 6)
    for dim, blocks in cuts:
        draws = jnp.exp(jax.random.uniform(jax.random.fold_in(own, dim), (blocks,), jnp.float32, least / len(cuts), high / len(cuts)))
        factor_of = factor_of * jnp.repeat(draws, extent[dim] // blocks).reshape([-1 if axis == dim else 1 for axis in range(len(extent))])
    return factor_of


def scatter_about(stream_key, dims, width, most, shards=(), kind=jnp.bfloat16):
    level = block_scale(stream_key, dims, shards, -0.22, 0.18) if shards else 1.0
    values = jax.random.normal(stream_key, dims, jnp.float32) * width * level
    return jnp.minimum(jnp.maximum(values, -most), most).astype(kind)


def setup_inputs(seed: int = 0, part: int = 0) -> dict:
    splits = jax.random.split(jax.random.key(seed), 13)
    own_keys = jax.random.split(jax.random.fold_in(splits[12], part), 13)
    return {
        "latent": draw_latent(jax.random.fold_in(jax.random.fold_in(splits[12], part), 71), part),
        "context": scatter_about(own_keys[1], (CTX, D), 1.0, 6.0, ((0, 4),)),
        "conditioning": scatter_about(own_keys[2], (D,), 1.5, 6.0, ((0, 4),)),
        "norm_gain": jnp.clip(1.0 + 0.18 * jax.random.normal(splits[3], (D,), jnp.float32), 0.1, 1.9),
        "shift_weight": scatter_about(splits[4], (D, D), D ** -0.5, 0.09375, ((0, 4), (1, 4))),
        "scale_weight": scatter_about(splits[5], (D, D), D ** -0.5, 0.09375, ((0, 4), (1, 4))),
        "gate_weight": scatter_about(splits[6], (D, D), D ** -0.5, 0.09375, ((0, 4), (1, 4))),
        "query_weight": draw_query_weight(jax.random.fold_in(splits[12], 71), part),
        "key_weight": draw_key_weight(jax.random.fold_in(splits[12], 71), part),
        "value_weight": scatter_about(splits[9], (D, KV_HEADS * HD), D ** -0.5, 0.09375, ((1, 4),)),
        "out_weight": scatter_about(splits[10], (HEADS * HD, D), (HD // 4) ** -0.5, 1.5, ((1, 4),)),
        "sink_logit": jnp.clip(3.0 + 4.0 * jax.random.uniform(splits[11], (HEADS,), jnp.float32) ** block_scale(splits[11], (HEADS,), ((0, 4),), -0.2, 0.2), 3.0, 7.0),
    }


epsilon = 1e-06
rope_base = 10000.0
neg_large = -1e+30

def row_norm(matrix, norm_gain):
    values = matrix.astype(jnp.float32)
    return values * lax.rsqrt(lax.optimization_barrier(jnp.mean(values * values, axis=-1, keepdims=True)) + epsilon) * norm_gain

def axial_turn(values, position):
    half_dim = values.shape[-1] // 2
    quarter = half_dim // 2
    inverse = rope_base ** (-jnp.arange(quarter, dtype=jnp.float32) / quarter)

    def turn(section, coordinate):
        angles = coordinate.astype(jnp.float32)[:, None] * inverse[None, :]
        cosine = jnp.cos(angles)[:, None, :]
        sine_part = jnp.sin(angles)[:, None, :]
        leading = section[..., :quarter]
        trailing = section[..., quarter:]
        return jnp.concatenate([leading * cosine - trailing * sine_part, leading * sine_part + trailing * cosine], axis=-1)
    return jnp.concatenate([turn(values[..., :half_dim], position // GRID_W), turn(values[..., half_dim:], position % GRID_W)], axis=-1)

def reference(latent, context, conditioning, norm_gain, shift_weight, scale_weight, gate_weight, query_weight, key_weight, value_weight, out_weight, sink_logit):
    lifted = jax.nn.silu(conditioning.astype(jnp.float32)).astype(jnp.bfloat16)[None, :]
    shift_vec = jnp.dot(lifted, shift_weight, preferred_element_type=jnp.float32)[0]
    scale_vec = jnp.dot(lifted, scale_weight, preferred_element_type=jnp.float32)[0]
    gate_vec = jnp.dot(lifted, gate_weight, preferred_element_type=jnp.float32)[0]
    normed = (row_norm(latent, norm_gain) * (1.0 + scale_vec) + shift_vec).astype(jnp.bfloat16)
    position = jnp.arange(SEQ, dtype=jnp.int32)
    queries = axial_turn(jnp.dot(normed, query_weight, preferred_element_type=jnp.float32).reshape(SEQ, HEADS, HD), position).astype(jnp.bfloat16)
    latent_keys = axial_turn(jnp.dot(normed, key_weight, preferred_element_type=jnp.float32).reshape(SEQ, KV_HEADS, HD), position).astype(jnp.bfloat16)
    latent_values = jnp.dot(normed, value_weight, preferred_element_type=jnp.float32).astype(jnp.bfloat16).reshape(SEQ, KV_HEADS, HD)
    prepared = row_norm(context, norm_gain).astype(jnp.bfloat16)
    context_keys = jnp.dot(prepared, key_weight, preferred_element_type=jnp.float32).astype(jnp.bfloat16).reshape(CTX, KV_HEADS, HD).astype(jnp.float32)
    context_values = jnp.dot(prepared, value_weight, preferred_element_type=jnp.float32).astype(jnp.bfloat16).reshape(CTX, KV_HEADS, HD).astype(jnp.float32)
    group_size = HEADS // KV_HEADS
    factor = HD ** (-0.5)
    padded_keys = jnp.pad(latent_keys, ((WIN, WIN), (0, 0), (0, 0)))
    padded_values = jnp.pad(latent_values, ((WIN, WIN), (0, 0), (0, 0)))
    sink_values = sink_logit.astype(jnp.float32).reshape(KV_HEADS, group_size)[:, :, None, None]

    def one_block(block_index):
        first_row = block_index * WIN
        block_queries = lax.dynamic_slice_in_dim(queries, first_row, WIN, 0).reshape(WIN, KV_HEADS, group_size, HD).astype(jnp.float32)
        block_keys = lax.dynamic_slice_in_dim(padded_keys, first_row, 3 * WIN, 0).astype(jnp.float32)
        block_values = lax.dynamic_slice_in_dim(padded_values, first_row, 3 * WIN, 0).astype(jnp.float32)
        local_scores = jnp.einsum('qhgd,khd->hgqk', block_queries, block_keys) * factor
        query_pos = first_row + jnp.arange(WIN, dtype=jnp.int32)
        key_pos = first_row - WIN + jnp.arange(3 * WIN, dtype=jnp.int32)
        allowed = (jnp.abs(key_pos[None, :] - query_pos[:, None]) <= WIN) & (key_pos[None, :] >= 0) & (key_pos[None, :] < SEQ)
        local_scores = jnp.where(allowed, local_scores, neg_large)
        context_scores = jnp.einsum('qhgd,thd->hgqt', block_queries, context_keys) * factor
        joined = jnp.concatenate([local_scores, context_scores, jnp.broadcast_to(sink_values, local_scores.shape[:-1] + (1,))], axis=-1)
        highest = lax.optimization_barrier(jnp.max(joined, axis=-1, keepdims=True))
        exponent = jnp.exp(joined - highest)
        weights = (exponent / lax.optimization_barrier(jnp.sum(exponent, axis=-1, keepdims=True))).astype(jnp.bfloat16)
        weights = lax.optimization_barrier(weights).astype(jnp.float32)
        out_block = jnp.einsum('hgqk,khd->qhgd', weights[..., :3 * WIN], block_values) + jnp.einsum('hgqt,thd->qhgd', weights[..., 3 * WIN:3 * WIN + CTX], context_values)
        return out_block.reshape(WIN, HEADS * HD).astype(jnp.bfloat16)
    attended = lax.map(one_block, jnp.arange(SEQ // WIN, dtype=jnp.int32)).reshape(SEQ, HEADS * HD)
    blended = jnp.dot(attended, out_weight, preferred_element_type=jnp.float32).astype(jnp.bfloat16)
    blended = lax.optimization_barrier(blended).astype(jnp.float32)
    return (latent.astype(jnp.float32) + gate_vec * blended).astype(jnp.bfloat16)
```

```python
import functools

import jax
import jax.numpy as jnp
from jax import lax
from jax.experimental import pallas as pl
from jax.experimental.pallas import tpu as pltpu
from jax.sharding import PartitionSpec as P

HEADS = 16
KV_HEADS = 8
HD = 64
GRID_W = 64
WIN = 128
LANES = 128
CORES = 2

epsilon = 1e-06
rope_base = 10000.0
neg_large = -1e30


VMEM = pl.BlockSpec(memory_space=pltpu.VMEM)
SMEM = pl.BlockSpec(memory_space=pltpu.SMEM)


def cost(flops, traffic):
    return pl.CostEstimate(flops=int(flops), bytes_accessed=int(traffic), transcendentals=0)


def row_norm(matrix, norm_gain):
    values = matrix.astype(jnp.float32)
    return (
        values * lax.rsqrt(jnp.mean(values * values, axis=-1, keepdims=True) + epsilon) * norm_gain
    )


def from_chip(block, count, step):
    chips = count // CORES
    perm = [
        (((t // CORES + step) % chips) * CORES + t % CORES, t) for t in range(count)
    ]
    return lax.ppermute(block, "tp", perm)


def from_partner(block, count):
    return lax.ppermute(block, "tp", [(t ^ 1, t) for t in range(count)])


def send_rows(block, count, step, flip):
    chips = count // CORES
    perm = [
        (t, ((t // CORES + step) % chips) * CORES + (t % CORES) ^ flip) for t in range(count)
    ]
    return lax.ppermute(block, "tp", perm)


def turn_tables(position):
    lane = jnp.arange(LANES, dtype=jnp.int32)
    quarter = HD // 4
    inverse = rope_base ** (-(lane % quarter).astype(jnp.float32) / quarter)
    by_row = (lane % HD) < HD // 2
    coordinate = jnp.where(
        by_row[None, :], (position // GRID_W)[:, None], (position % GRID_W)[:, None]
    )
    angles = coordinate.astype(jnp.float32) * inverse[None, :]
    sign = jnp.where(lane % (HD // 2) < quarter, -1.0, 1.0)
    return jnp.cos(angles), jnp.sin(angles) * sign[None, :]


def project_kernel(parts, carried, place, *refs):
    x_refs = refs[:parts]
    gain, shift, wq, wkv, cosine, sine = refs[parts : parts + 6]
    rest = refs[parts + 6 :]
    if carried:
        q_prev, kv_prev, q_out, kv_out = rest
        q_out[...] = q_prev[...]
        kv_out[...] = kv_prev[...]
    else:
        q_out, kv_out = rest
    depth = wq.shape[0]
    step = min(depth, 512)
    rows = x_refs[0].shape[0]
    query_width = wq.shape[1]
    key_width = wkv.shape[1] // 2
    roots = []
    for ref in x_refs:
        total = jnp.zeros((rows, LANES), jnp.float32)
        for k in range(0, depth, step):
            v = ref[:, k : k + step].astype(jnp.float32)
            v = v * v
            for c in range(0, step, LANES):
                total = total + v[:, c : c + LANES]
        roots.append(lax.rsqrt(jnp.sum(total, axis=1, keepdims=True) / depth + epsilon))
    acc_q = jnp.zeros((rows * parts, query_width), jnp.float32)
    acc_kv = jnp.zeros((rows * parts, 2 * key_width), jnp.float32)
    for k in range(0, depth, step):
        pieces = []
        for ref, root in zip(x_refs, roots):
            v = ref[:, k : k + step].astype(jnp.float32) * root
            v = v * gain[:, k : k + step] + shift[:, k : k + step]
            pieces.append(v.astype(jnp.bfloat16))
        normed = jnp.concatenate(pieces, axis=0)
        acc_q = acc_q + jnp.dot(
            normed, wq[k : k + step, :], preferred_element_type=jnp.float32
        )
        acc_kv = acc_kv + jnp.dot(
            normed, wkv[k : k + step, :], preferred_element_type=jnp.float32
        )
    lane = lax.broadcasted_iota(jnp.int32, (rows, LANES), 1)
    first = lane % (HD // 2) < HD // 4
    for i in range(parts):
        start = pl.multiple_of(place[i], 16)
        cos_rows = cosine[pl.ds(start, rows), :]
        sin_rows = sine[pl.ds(start, rows), :]
        for acc, out, width in (
            (acc_q, q_out, query_width),
            (acc_kv, kv_out, key_width),
        ):
            block = acc[i * rows : (i + 1) * rows]
            for c in range(0, block.shape[1], LANES):
                piece = block[:, c : c + LANES]
                turned = min(max(width - c, 0), LANES)
                if turned:
                    other = jnp.where(
                        first,
                        pltpu.roll(piece, LANES - HD // 4, 1),
                        pltpu.roll(piece, HD // 4, 1),
                    )
                    moved = piece * cos_rows + other * sin_rows
                    piece = moved if turned == LANES else jnp.where(lane < turned, moved, piece)
                out[pl.ds(start, rows), c : c + LANES] = piece.astype(jnp.bfloat16)


def project(blocks, places, gain, shift, wq, wkv, tables, carried, out_rows):
    parts = len(blocks)
    depth, query_width = wq.shape
    kv_width = wkv.shape[1]
    rows = blocks[0].shape[0] * parts
    return pl.pallas_call(
        functools.partial(project_kernel, parts, bool(carried)),
        out_shape=(
            jax.ShapeDtypeStruct((out_rows, query_width), jnp.bfloat16),
            jax.ShapeDtypeStruct((out_rows, kv_width), jnp.bfloat16),
        ),
        in_specs=[SMEM] + [VMEM] * (parts + 6 + len(carried)),
        out_specs=(VMEM, VMEM),
        compiler_params=pltpu.CompilerParams(vmem_limit_bytes=40 * 1024 * 1024),
        cost_estimate=cost(
            2 * rows * depth * (query_width + kv_width), 2 * depth * (rows + query_width + kv_width)
        ),
    )(jnp.stack(places), *blocks, gain, shift, wq, wkv, *tables, *carried)


def attend_block(q, band, ctx_refs, sink, out, out_row, low, high):
    query_width = q.shape[1]
    key_width = ctx_refs[0].shape[1] // 2
    group = HEADS // KV_HEADS
    row = lax.broadcasted_iota(jnp.int32, (WIN, WIN), 0)
    col = lax.broadcasted_iota(jnp.int32, (WIN, WIN), 1)
    before = col >= row
    after = col <= row
    if low is not None:
        before = before & (low != 0)
    if high is not None:
        after = after & (high != 0)
    before = jnp.concatenate([before] * group, axis=0)
    after = jnp.concatenate([after] * group, axis=0)
    contract = (((1,), (1,)), ((), ()))
    for head in range(key_width // HD):
        base = head * group * HD
        query = jnp.concatenate(
            [q[:, base + g * HD : base + (g + 1) * HD] for g in range(group)], axis=0
        )
        query = query * jnp.asarray(HD**-0.5, jnp.bfloat16)
        ks = slice(head * HD, (head + 1) * HD)
        vs = slice(key_width + head * HD, key_width + (head + 1) * HD)
        scores = [
            lax.dot_general(
                query, ref[r : r + WIN, ks], contract, preferred_element_type=jnp.float32
            )
            for ref, r in band
        ] + [
            lax.dot_general(query, ref[:, ks], contract, preferred_element_type=jnp.float32)
            for ref in ctx_refs
        ]
        scores[0] = jnp.where(before, scores[0], neg_large)
        scores[2] = jnp.where(after, scores[2], neg_large)
        sinks = jnp.concatenate(
            [jnp.full((WIN, 1), sink[head * group + g], jnp.float32) for g in range(group)], axis=0
        )
        top = sinks
        for s in scores:
            top = jnp.maximum(top, jnp.max(s, axis=1, keepdims=True))
        powers = [jnp.exp(s - top) for s in scores]
        total = jnp.exp(sinks - top)
        for p in powers:
            total = total + jnp.sum(p, axis=1, keepdims=True)
        inverse = 1.0 / total
        weights = [(p * inverse).astype(jnp.bfloat16) for p in powers]
        values = [ref[r : r + WIN, vs] for ref, r in band] + [ref[:, vs] for ref in ctx_refs]
        gathered = jnp.zeros((group * WIN, HD), jnp.float32)
        for w, v in zip(weights, values):
            gathered = gathered + jnp.dot(w, v, preferred_element_type=jnp.float32)
        for g in range(group):
            out[out_row : out_row + WIN, base + g * HD : base + (g + 1) * HD] = gathered[
                g * WIN : (g + 1) * WIN
            ].astype(jnp.bfloat16)


def inner_kernel(blocks, sink, q, kv, *refs):
    ctx, out = refs[:-1], refs[-1]
    for n in range(1, blocks - 1):
        band = [(kv, (n + s) * WIN) for s in (-1, 0, 1)]
        attend_block(
            q[n * WIN : (n + 1) * WIN, :], band, ctx, sink, out, (n - 1) * WIN, None, None
        )


def edge_kernel(blocks, inner, ends, sink, q, kv, head, tail, *refs):
    if inner:
        ctx, middle, out = refs[:-2], refs[-2], refs[-1]
        out[WIN : (blocks - 1) * WIN, :] = middle[...]
    else:
        ctx, out = refs[:-1], refs[-1]
    for n in sorted({0, blocks - 1}):
        band = [
            (head, 0) if n == 0 else (kv, (n - 1) * WIN),
            (kv, n * WIN),
            (tail, 0) if n == blocks - 1 else (kv, (n + 1) * WIN),
        ]
        attend_block(
            q[n * WIN : (n + 1) * WIN, :],
            band,
            ctx,
            sink,
            out,
            n * WIN,
            ends[0] if n == 0 else None,
            ends[1] if n == blocks - 1 else None,
        )


def attend_cost(blocks, query_width, ctx):
    keys = 3 * WIN + sum(c.shape[0] for c in ctx)
    return cost(4 * blocks * WIN * keys * query_width * 4, 2**20)


def out_kernel(parts, rows, place, *refs):
    att, weight, outs = refs[:parts], refs[parts], refs[parts + 1 :]
    width = att[0].shape[1]
    pieces = []
    for i in range(len(outs)):
        start = pl.multiple_of(place[i], 16)
        total = jnp.zeros((rows, weight.shape[1]), jnp.float32)
        for k in range(parts):
            total = total + jnp.dot(
                att[k][pl.ds(start, rows), :],
                weight[k * width : (k + 1) * width, :],
                preferred_element_type=jnp.float32,
            )
        outs[i][...] = total.astype(jnp.bfloat16)


def out_rows(att, weight, places, rows):
    parts = len(att)
    count = len(places)
    return pl.pallas_call(
        functools.partial(out_kernel, parts, rows),
        out_shape=tuple(
            jax.ShapeDtypeStruct((rows, weight.shape[1]), jnp.bfloat16) for _ in range(count)
        ),
        in_specs=[SMEM] + [VMEM] * (parts + 1),
        out_specs=tuple(VMEM for _ in range(count)),
        compiler_params=pltpu.CompilerParams(vmem_limit_bytes=32 * 1024 * 1024),
        cost_estimate=cost(2 * rows * count * weight.shape[0] * weight.shape[1], 2**22),
    )(jnp.stack(places), *att, weight)


def finish_kernel(parts, place, latent, gate, *refs):
    blends, out = refs[:parts], refs[parts]
    width = blends[0].shape[1]
    for i in range(parts):
        cols = pl.ds(pl.multiple_of(place[i], LANES), width)
        out[:, cols] = (
            latent[:, cols].astype(jnp.float32)
            + gate[:, cols] * blends[i][...].astype(jnp.float32)
        ).astype(jnp.bfloat16)


def local(
    latent,
    context,
    conditioning,
    norm_gain,
    shift_weight,
    scale_weight,
    gate_weight,
    query_weight,
    key_weight,
    value_weight,
    out_weight,
    sink_logit,
):
    count = lax.axis_size("tp")
    chips = count // CORES
    me = lax.axis_index("tp")
    chip, core = me // CORES, me % CORES
    ring = lax.axis_size("sp")
    rank = lax.axis_index("sp")
    rows, depth = latent.shape
    row_count = rows * count
    cuts = 2
    piece = rows // cuts

    def index(step, flip):
        return ((chip + step) % chips) * CORES + (core ^ flip)

    near = [latent, from_partner(latent, count)]
    near_place = [index(0, 0) * rows, index(0, 1) * rows]
    far, far_place = [], []
    for step in range(1, chips):
        for cut in range(cuts):
            got = from_chip(latent[cut * piece : (cut + 1) * piece], count, step)
            far += [got, from_partner(got, count)]
            far_place += [index(step, flip) * rows + cut * piece for flip in (0, 1)]

    lifted = jax.nn.silu(conditioning.astype(jnp.float32)).astype(jnp.bfloat16)[None, :]
    partial = jnp.concatenate(
        [
            jnp.dot(lifted, w, preferred_element_type=jnp.float32)
            for w in (shift_weight, scale_weight, gate_weight)
        ],
        axis=0,
    )
    summed = jnp.sum(lax.all_gather(partial, "sp", axis=0), axis=0)
    vectors = lax.all_gather(summed, "tp", axis=1, tiled=True)
    shift_vec = vectors[0:1]
    gain_vec = norm_gain[None, :] * (1.0 + vectors[1:2])
    gate_vec = vectors[2:3]

    kv_weight = jnp.concatenate([key_weight, value_weight], axis=1)
    prepared = row_norm(context, norm_gain).astype(jnp.bfloat16)
    own = jnp.dot(prepared, kv_weight, preferred_element_type=jnp.float32).astype(jnp.bfloat16)
    if ring <= 8:
        ctx = [own] + [
            lax.ppermute(own, "sp", [((i + d) % ring, i) for i in range(ring)])
            for d in range(1, ring)
        ]
    else:
        ctx = [lax.all_gather(own, "sp", axis=0, tiled=True)]

    row_offset = rank * row_count
    tables = turn_tables(row_offset + jnp.arange(row_count, dtype=jnp.int32))
    args = (gain_vec, shift_vec, query_weight, kv_weight, tables)
    queries, key_value = project(near, near_place, *args, (), row_count)
    if far:
        queries, key_value = project(
            far, far_place, *args, (queries, key_value), row_count
        )

    head = lax.ppermute(
        key_value[row_count - WIN :], "sp", [(i, i + 1) for i in range(ring - 1)]
    )
    tail = lax.ppermute(key_value[:WIN], "sp", [(i + 1, i) for i in range(ring - 1)])
    blocks = row_count // WIN
    query_width = query_weight.shape[1]
    limit = pltpu.CompilerParams(vmem_limit_bytes=32 * 1024 * 1024)
    middle = ()
    if blocks > 2:
        middle = (
            pl.pallas_call(
                functools.partial(inner_kernel, blocks),
                out_shape=jax.ShapeDtypeStruct(((blocks - 2) * WIN, query_width), jnp.bfloat16),
                in_specs=[SMEM] + [VMEM] * (2 + len(ctx)),
                out_specs=VMEM,
                compiler_params=limit,
                cost_estimate=attend_cost(blocks - 2, query_width, ctx),
            )(sink_logit, queries, key_value, *ctx),
        )
    ends = jnp.stack([(rank > 0).astype(jnp.int32), (rank < ring - 1).astype(jnp.int32)])
    attended = pl.pallas_call(
        functools.partial(edge_kernel, blocks, bool(middle)),
        out_shape=jax.ShapeDtypeStruct((row_count, query_width), jnp.bfloat16),
        in_specs=[SMEM, SMEM] + [VMEM] * (4 + len(ctx) + len(middle)),
        out_specs=VMEM,
        compiler_params=limit,
        cost_estimate=attend_cost(2, query_width, ctx),
    )(ends, sink_logit, queries, key_value, head, tail, *ctx, *middle)

    att, order = [], []
    for step in range(chips):
        got = attended if step == 0 else from_chip(attended, count, step)
        att += [got, from_partner(got, count)]
        order += [index(step, 0), index(step, 1)]
    weight = jnp.concatenate(
        [
            lax.dynamic_slice_in_dim(out_weight, source * query_width, query_width, 0)
            for source in order
        ],
        axis=0,
    )

    steps = [(step, flip) for step in range(1, chips) for flip in range(CORES)]
    received, places = [], []
    if steps:
        sent = out_rows(att, weight, [index(s, f) * rows for s, f in steps], rows)
        for (s, f), block in zip(steps, sent):
            received.append(send_rows(block, count, s, f))
            places.append((((chip - s) % chips) * CORES + (core ^ f)) * weight.shape[1])
    mine, other = out_rows(att, weight, [index(0, 0) * rows, index(0, 1) * rows], rows)
    received += [mine, from_partner(other, count)]
    places += [index(0, 0) * weight.shape[1], index(0, 1) * weight.shape[1]]
    return pl.pallas_call(
        functools.partial(finish_kernel, count),
        out_shape=jax.ShapeDtypeStruct((rows, depth), jnp.bfloat16),
        in_specs=[SMEM] + [VMEM] * (2 + count),
        out_specs=VMEM,
        compiler_params=limit,
        cost_estimate=cost(2**21, 2**22),
    )(jnp.stack(places), latent, gate_vec, *received)


def solution(mesh):
    in_specs = (
        P(("grp", "sp", "tp"), None),
        P(("grp", "sp"), None),
        P(("grp", "sp")),
        P(),
        P("sp", "tp"),
        P("sp", "tp"),
        P("sp", "tp"),
        P(None, "tp"),
        P(None, "tp"),
        P(None, "tp"),
        P(None, "tp"),
        P("tp"),
    )
    out_specs = P(("grp", "sp", "tp"), None)
    return jax.shard_map(local, mesh=mesh, in_specs=in_specs, out_specs=out_specs, check_vma=False)
```

```python
import functools

import jax
import jax.numpy as jnp
from jax import lax
from jax.experimental import pallas as pl
from jax.experimental.pallas import tpu as pltpu
from jax.sharding import PartitionSpec as P

HEADS = 16
KV_HEADS = 8
HD = 64
GRID_W = 64
WIN = 128
LANES = 128
CORES = 2

epsilon = 1e-06
rope_base = 10000.0
neg_large = -1e30


VMEM = pl.BlockSpec(memory_space=pltpu.VMEM)
SMEM = pl.BlockSpec(memory_space=pltpu.SMEM)


def cost(flops, traffic):
    return pl.CostEstimate(flops=int(flops), bytes_accessed=int(traffic), transcendentals=0)


def from_chip(block, count, step):
    chips = count // CORES
    perm = [
        (((t // CORES + step) % chips) * CORES + t % CORES, t) for t in range(count)
    ]
    return lax.ppermute(block, "tp", perm)


def from_partner(block, count):
    return lax.ppermute(block, "tp", [(t ^ 1, t) for t in range(count)])


def send_rows(block, count, step, flip):
    chips = count // CORES
    perm = [
        (t, ((t // CORES + step) % chips) * CORES + (t % CORES) ^ flip) for t in range(count)
    ]
    return lax.ppermute(block, "tp", perm)


def turn_tables(position):
    lane = jnp.arange(LANES, dtype=jnp.int32)
    quarter = HD // 4
    inverse = rope_base ** (-(lane % quarter).astype(jnp.float32) / quarter)
    by_row = (lane % HD) < HD // 2
    coordinate = jnp.where(
        by_row[None, :], (position // GRID_W)[:, None], (position % GRID_W)[:, None]
    )
    angles = coordinate.astype(jnp.float32) * inverse[None, :]
    sign = jnp.where(lane % (HD // 2) < quarter, -1.0, 1.0)
    return jnp.cos(angles), jnp.sin(angles) * sign[None, :]


def row_root(ref, step):
    rows, depth = ref.shape
    total = jnp.zeros((rows, LANES), jnp.float32)
    for k in range(0, depth, step):
        v = ref[:, k : k + step].astype(jnp.float32)
        v = v * v
        for c in range(0, step, LANES):
            total = total + v[:, c : c + LANES]
    return lax.rsqrt(jnp.sum(total, axis=1, keepdims=True) / depth + epsilon)


def context_kernel(context, gain, wk, wv, out):
    depth = wk.shape[0]
    step = min(depth, 512)
    root = row_root(context, step)
    acc = jnp.zeros(out.shape, jnp.float32)
    for k in range(0, depth, step):
        v = context[:, k : k + step].astype(jnp.float32) * root * gain[:, k : k + step]
        wkv = jnp.concatenate([wk[k : k + step, :], wv[k : k + step, :]], axis=1)
        acc = acc + jnp.dot(v.astype(jnp.bfloat16), wkv, preferred_element_type=jnp.float32)
    out[...] = acc.astype(jnp.bfloat16)


def project_kernel(parts, carried, place, *refs):
    x_refs = refs[:parts]
    gain, shift, wq, wk, wv, cosine, sine = refs[parts : parts + 7]
    rest = refs[parts + 7 :]
    if carried:
        q_prev, kv_prev, q_out, kv_out = rest
        q_out[...] = q_prev[...]
        kv_out[...] = kv_prev[...]
    else:
        q_out, kv_out = rest
    depth = wq.shape[0]
    step = min(depth, 512)
    rows = x_refs[0].shape[0]
    query_width = wq.shape[1]
    key_width = wk.shape[1]
    roots = []
    for ref in x_refs:
        roots.append(row_root(ref, step))
    acc_q = jnp.zeros((rows * parts, query_width), jnp.float32)
    acc_kv = jnp.zeros((rows * parts, 2 * key_width), jnp.float32)
    for k in range(0, depth, step):
        pieces = []
        for ref, root in zip(x_refs, roots):
            v = ref[:, k : k + step].astype(jnp.float32) * root
            v = v * gain[:, k : k + step] + shift[:, k : k + step]
            pieces.append(v.astype(jnp.bfloat16))
        normed = jnp.concatenate(pieces, axis=0)
        acc_q = acc_q + jnp.dot(
            normed, wq[k : k + step, :], preferred_element_type=jnp.float32
        )
        wkv = jnp.concatenate([wk[k : k + step, :], wv[k : k + step, :]], axis=1)
        acc_kv = acc_kv + jnp.dot(normed, wkv, preferred_element_type=jnp.float32)
    lane = lax.broadcasted_iota(jnp.int32, (rows, LANES), 1)
    first = lane % (HD // 2) < HD // 4
    for i in range(parts):
        start = pl.multiple_of(place[i], 16)
        cos_rows = cosine[pl.ds(start, rows), :]
        sin_rows = sine[pl.ds(start, rows), :]
        for acc, out, width in (
            (acc_q, q_out, query_width),
            (acc_kv, kv_out, key_width),
        ):
            block = acc[i * rows : (i + 1) * rows]
            for c in range(0, block.shape[1], LANES):
                piece = block[:, c : c + LANES]
                turned = min(max(width - c, 0), LANES)
                if turned:
                    other = jnp.where(
                        first,
                        pltpu.roll(piece, LANES - HD // 4, 1),
                        pltpu.roll(piece, HD // 4, 1),
                    )
                    moved = piece * cos_rows + other * sin_rows
                    piece = moved if turned == LANES else jnp.where(lane < turned, moved, piece)
                out[pl.ds(start, rows), c : c + LANES] = piece.astype(jnp.bfloat16)


def project(blocks, places, gain, shift, wq, wk, wv, tables, carried, out_rows):
    parts = len(blocks)
    depth, query_width = wq.shape
    kv_width = 2 * wk.shape[1]
    rows = blocks[0].shape[0] * parts
    return pl.pallas_call(
        functools.partial(project_kernel, parts, bool(carried)),
        out_shape=(
            jax.ShapeDtypeStruct((out_rows, query_width), jnp.bfloat16),
            jax.ShapeDtypeStruct((out_rows, kv_width), jnp.bfloat16),
        ),
        in_specs=[SMEM] + [VMEM] * (parts + 7 + len(carried)),
        out_specs=(VMEM, VMEM),
        compiler_params=pltpu.CompilerParams(vmem_limit_bytes=24 * 1024 * 1024),
        cost_estimate=cost(
            2 * rows * depth * (query_width + kv_width), 2 * depth * (rows + query_width + kv_width)
        ),
    )(jnp.stack(places), *blocks, gain, shift, wq, wk, wv, *tables, *carried)


def attend_block(q, band, ctx_refs, sink, out, out_row, low, high):
    key_width = ctx_refs[0].shape[1] // 2
    group = HEADS // KV_HEADS
    row = lax.broadcasted_iota(jnp.int32, (WIN, WIN), 0)
    col = lax.broadcasted_iota(jnp.int32, (WIN, WIN), 1)
    before = col >= row
    after = col <= row
    if low is not None:
        before = before & (low != 0)
    if high is not None:
        after = after & (high != 0)
    before = jnp.concatenate([before] * group, axis=0)
    after = jnp.concatenate([after] * group, axis=0)
    contract = (((1,), (1,)), ((), ()))
    for head in range(key_width // HD):
        base = head * group * HD
        query = jnp.concatenate(
            [q[:, base + g * HD : base + (g + 1) * HD] for g in range(group)], axis=0
        )
        query = query * jnp.asarray(HD**-0.5, jnp.bfloat16)
        ks = slice(head * HD, (head + 1) * HD)
        vs = slice(key_width + head * HD, key_width + (head + 1) * HD)
        scores = [
            lax.dot_general(
                query, ref[r : r + WIN, ks], contract, preferred_element_type=jnp.float32
            )
            for ref, r in band
        ] + [
            lax.dot_general(query, ref[:, ks], contract, preferred_element_type=jnp.float32)
            for ref in ctx_refs
        ]
        scores[0] = jnp.where(before, scores[0], neg_large)
        scores[2] = jnp.where(after, scores[2], neg_large)
        sinks = jnp.concatenate(
            [jnp.full((WIN, 1), sink[head * group + g], jnp.float32) for g in range(group)], axis=0
        )
        top = sinks
        for s in scores:
            top = jnp.maximum(top, jnp.max(s, axis=1, keepdims=True))
        values = [ref[r : r + WIN, vs] for ref, r in band] + [ref[:, vs] for ref in ctx_refs]
        gathered = jnp.zeros((group * WIN, 2 * HD), jnp.float32)
        for s, v in zip(scores, values):
            power = jnp.exp(s - top).astype(jnp.bfloat16)
            joined = jnp.concatenate([v, jnp.ones_like(v)], axis=1)
            gathered = gathered + jnp.dot(power, joined, preferred_element_type=jnp.float32)
        total = gathered[:, HD : HD + 1] + jnp.exp(sinks - top)
        gathered = gathered[:, :HD] * (1.0 / total)
        for g in range(group):
            out[out_row : out_row + WIN, base + g * HD : base + (g + 1) * HD] = gathered[
                g * WIN : (g + 1) * WIN
            ].astype(jnp.bfloat16)


def inner_kernel(blocks, sink, q, kv, *refs):
    ctx, out = refs[:-1], refs[-1]
    for n in range(1, blocks - 1):
        band = [(kv, (n + s) * WIN) for s in (-1, 0, 1)]
        attend_block(
            q[n * WIN : (n + 1) * WIN, :], band, ctx, sink, out, (n - 1) * WIN, None, None
        )


def edge_kernel(blocks, inner, ends, sink, q, kv, head, tail, *refs):
    if inner:
        ctx, middle, out = refs[:-2], refs[-2], refs[-1]
        out[WIN : (blocks - 1) * WIN, :] = middle[...]
    else:
        ctx, out = refs[:-1], refs[-1]
    for n in sorted({0, blocks - 1}):
        band = [
            (head, 0) if n == 0 else (kv, (n - 1) * WIN),
            (kv, n * WIN),
            (tail, 0) if n == blocks - 1 else (kv, (n + 1) * WIN),
        ]
        attend_block(
            q[n * WIN : (n + 1) * WIN, :],
            band,
            ctx,
            sink,
            out,
            n * WIN,
            ends[0] if n == 0 else None,
            ends[1] if n == blocks - 1 else None,
        )


def attend_cost(blocks, query_width, ctx):
    keys = 3 * WIN + sum(c.shape[0] for c in ctx)
    return cost(4 * blocks * WIN * keys * query_width * 4, 2**20)


def out_kernel(parts, rows, place, *refs):
    att, weight, outs = refs[:parts], refs[parts], refs[parts + 1 :]
    width = att[0].shape[1]
    for i in range(len(outs)):
        start = pl.multiple_of(place[i], 16)
        total = jnp.zeros((rows, weight.shape[1]), jnp.float32)
        for k in range(parts):
            total = total + jnp.dot(
                att[k][pl.ds(start, rows), :],
                weight[k * width : (k + 1) * width, :],
                preferred_element_type=jnp.float32,
            )
        outs[i][...] = total.astype(jnp.bfloat16)


def out_rows(att, weight, places, rows):
    parts = len(att)
    count = len(places)
    return pl.pallas_call(
        functools.partial(out_kernel, parts, rows),
        out_shape=tuple(
            jax.ShapeDtypeStruct((rows, weight.shape[1]), jnp.bfloat16) for _ in range(count)
        ),
        in_specs=[SMEM] + [VMEM] * (parts + 1),
        out_specs=tuple(VMEM for _ in range(count)),
        compiler_params=pltpu.CompilerParams(vmem_limit_bytes=16 * 1024 * 1024),
        cost_estimate=cost(2 * rows * count * weight.shape[0] * weight.shape[1], 2**22),
    )(jnp.stack(places), *att, weight)


def finish_kernel(place, latent, gate, blend, *refs):
    refs[-1][...] = (
        latent[...].astype(jnp.float32) + gate[...] * blend[...].astype(jnp.float32)
    ).astype(jnp.bfloat16)


def finish(latent, gate, blend, place, mixed):
    rows, width = blend.shape
    there = pl.BlockSpec((rows, width), lambda i, place: (0, place[0]))
    here = pl.BlockSpec((rows, width), lambda i, place: (0, 0))
    line = pl.BlockSpec((1, width), lambda i, place: (0, place[0]))
    return pl.pallas_call(
        finish_kernel,
        out_shape=jax.ShapeDtypeStruct(latent.shape, jnp.bfloat16),
        grid_spec=pltpu.PrefetchScalarGridSpec(
            num_scalar_prefetch=1,
            grid=(1,),
            in_specs=[there, line, here] + [pl.BlockSpec(memory_space=pl.ANY)] * len(mixed),
            out_specs=there,
        ),
        input_output_aliases={4: 0} if mixed else {},
        compiler_params=pltpu.CompilerParams(vmem_limit_bytes=8 * 1024 * 1024),
        cost_estimate=cost(2**20, 2**20),
    )(place[None], latent, gate, blend, *mixed)


def local(
    latent,
    context,
    conditioning,
    norm_gain,
    shift_weight,
    scale_weight,
    gate_weight,
    query_weight,
    key_weight,
    value_weight,
    out_weight,
    sink_logit,
):
    count = lax.axis_size("tp")
    chips = count // CORES
    me = lax.axis_index("tp")
    chip, core = me // CORES, me % CORES
    ring = lax.axis_size("sp")
    rank = lax.axis_index("sp")
    rows, depth = latent.shape
    row_count = rows * count
    cuts = 2
    piece = rows // cuts

    def index(step, flip):
        return ((chip + step) % chips) * CORES + (core ^ flip)

    near = [latent, from_partner(latent, count)]
    near_place = [index(0, 0) * rows, index(0, 1) * rows]
    far, far_place = [], []
    for step in range(1, chips):
        for cut in range(cuts):
            got = from_chip(latent[cut * piece : (cut + 1) * piece], count, step)
            far += [got, from_partner(got, count)]
            far_place += [index(step, flip) * rows + cut * piece for flip in (0, 1)]

    lifted = jax.nn.silu(conditioning.astype(jnp.float32)).astype(jnp.bfloat16)[None, :]
    partial = jnp.concatenate(
        [
            jnp.dot(lifted, w, preferred_element_type=jnp.float32)
            for w in (shift_weight, scale_weight, gate_weight)
        ],
        axis=0,
    )
    summed = jnp.sum(lax.all_gather(partial, "sp", axis=0), axis=0)
    vectors = lax.all_gather(summed, "tp", axis=1, tiled=True)
    vectors, context, rank = lax.optimization_barrier((vectors, context, rank))
    shift_vec = vectors[0:1]
    gain_vec = norm_gain[None, :] * (1.0 + vectors[1:2])
    gate_vec = vectors[2:3]

    own = pl.pallas_call(
        context_kernel,
        out_shape=jax.ShapeDtypeStruct((context.shape[0], 2 * key_weight.shape[1]), jnp.bfloat16),
        in_specs=[VMEM] * 4,
        out_specs=VMEM,
        compiler_params=pltpu.CompilerParams(vmem_limit_bytes=16 * 1024 * 1024),
        cost_estimate=cost(4 * context.shape[0] * depth * key_weight.shape[1], 2**22),
    )(context, norm_gain[None, :], key_weight, value_weight)
    if ring <= 8:
        ctx = [own] + [
            lax.ppermute(own, "sp", [((i + d) % ring, i) for i in range(ring)])
            for d in range(1, ring)
        ]
    else:
        ctx = [lax.all_gather(own, "sp", axis=0, tiled=True)]

    row_offset = rank * row_count
    tables = turn_tables(row_offset + jnp.arange(row_count, dtype=jnp.int32))
    args = (gain_vec, shift_vec, query_weight, key_weight, value_weight, tables)
    queries, key_value = project(near, near_place, *args, (), row_count)
    if far:
        queries, key_value = project(
            far, far_place, *args, (queries, key_value), row_count
        )

    head = lax.ppermute(
        key_value[row_count - WIN :], "sp", [(i, i + 1) for i in range(ring - 1)]
    )
    tail = lax.ppermute(key_value[:WIN], "sp", [(i + 1, i) for i in range(ring - 1)])
    blocks = row_count // WIN
    query_width = query_weight.shape[1]
    limit = pltpu.CompilerParams(vmem_limit_bytes=16 * 1024 * 1024)
    middle = ()
    if blocks > 2:
        middle = (
            pl.pallas_call(
                functools.partial(inner_kernel, blocks),
                out_shape=jax.ShapeDtypeStruct(((blocks - 2) * WIN, query_width), jnp.bfloat16),
                in_specs=[SMEM] + [VMEM] * (2 + len(ctx)),
                out_specs=VMEM,
                compiler_params=limit,
                cost_estimate=attend_cost(blocks - 2, query_width, ctx),
            )(sink_logit, queries, key_value, *ctx),
        )
    ends = jnp.stack([(rank > 0).astype(jnp.int32), (rank < ring - 1).astype(jnp.int32)])
    attended = pl.pallas_call(
        functools.partial(edge_kernel, blocks, bool(middle)),
        out_shape=jax.ShapeDtypeStruct((row_count, query_width), jnp.bfloat16),
        in_specs=[SMEM, SMEM] + [VMEM] * (4 + len(ctx) + len(middle)),
        out_specs=VMEM,
        compiler_params=limit,
        cost_estimate=attend_cost(2, query_width, ctx),
    )(ends, sink_logit, queries, key_value, head, tail, *ctx, *middle)

    att, order = [], []
    for step in range(chips):
        got = attended if step == 0 else from_chip(attended, count, step)
        att += [got, from_partner(got, count)]
        order += [index(step, 0), index(step, 1)]
    weight = jnp.concatenate(
        [
            lax.dynamic_slice_in_dim(out_weight, source * query_width, query_width, 0)
            for source in order
        ],
        axis=0,
    )

    steps = [(step, flip) for step in range(1, chips) for flip in range(CORES)]
    received, places = [], []
    if steps:
        sent = out_rows(att, weight, [index(s, f) * rows for s, f in steps], rows)
        for (s, f), block in zip(steps, sent):
            received.append(send_rows(block, count, s, f))
            places.append((((chip - s) % chips) * CORES + (core ^ f)) )
    mine, other = out_rows(att, weight, [index(0, 0) * rows, index(0, 1) * rows], rows)
    near_blends = [(mine, index(0, 0)), (from_partner(other, count), index(0, 1))]
    mixed = ()
    for block, place in near_blends + list(zip(received, places)):
        mixed = (finish(latent, gate_vec, block, place, mixed),)
    return mixed[0]


def solution(mesh):
    in_specs = (
        P(("grp", "sp", "tp"), None),
        P(("grp", "sp"), None),
        P(("grp", "sp")),
        P(),
        P("sp", "tp"),
        P("sp", "tp"),
        P("sp", "tp"),
        P(None, "tp"),
        P(None, "tp"),
        P(None, "tp"),
        P(None, "tp"),
        P("tp"),
    )
    out_specs = P(("grp", "sp", "tp"), None)

    return jax.shard_map(local, mesh=mesh, in_specs=in_specs, out_specs=out_specs, check_vma=False)
```

```python
import functools

import jax
import jax.numpy as jnp
from jax import lax
from jax.experimental import pallas as pl
from jax.experimental.pallas import tpu as pltpu
from jax.sharding import PartitionSpec as P

HEADS = 16
KV_HEADS = 8
HD = 64
GRID_W = 64
WIN = 128
LANES = 128
CORES = 2

epsilon = 1e-06
rope_base = 10000.0
neg_large = -1e30


VMEM = pl.BlockSpec(memory_space=pltpu.VMEM)
SMEM = pl.BlockSpec(memory_space=pltpu.SMEM)


def cost(flops, traffic):
    return pl.CostEstimate(flops=int(flops), bytes_accessed=int(traffic), transcendentals=0)


def from_chip(block, count, step):
    chips = count // CORES
    perm = [
        (((t // CORES + step) % chips) * CORES + t % CORES, t) for t in range(count)
    ]
    return lax.ppermute(block, "tp", perm)


def from_partner(block, count):
    return lax.ppermute(block, "tp", [(t ^ 1, t) for t in range(count)])


def send_rows(block, count, step, flip):
    chips = count // CORES
    perm = [
        (t, ((t // CORES + step) % chips) * CORES + (t % CORES) ^ flip) for t in range(count)
    ]
    return lax.ppermute(block, "tp", perm)


def from_ring(block, ring):
    if ring > 8:
        gathered = lax.all_gather(block, "sp", axis=0)
        return [gathered[i] for i in range(ring)]
    return [block] + [
        lax.ppermute(block, "sp", [((i + d) % ring, i) for i in range(ring)])
        for d in range(1, ring)
    ]


def modulation_kernel(place, norm_gain, *refs):
    blocks, (gain, shift, gate) = refs[:-3], refs[-3:]
    width = blocks[0].shape[1]
    for i, block in enumerate(blocks):
        cols = pl.ds(pl.multiple_of(place[i], LANES), width)
        shift[:, cols] = block[0:1, :]
        gain[:, cols] = norm_gain[:, cols] * (1.0 + block[1:2, :])
        gate[:, cols] = block[2:3, :]


def turn_tables(position):
    lane = jnp.arange(LANES, dtype=jnp.int32)
    quarter = HD // 4
    inverse = rope_base ** (-(lane % quarter).astype(jnp.float32) / quarter)
    by_row = (lane % HD) < HD // 2
    coordinate = jnp.where(
        by_row[None, :], (position // GRID_W)[:, None], (position % GRID_W)[:, None]
    )
    angles = coordinate.astype(jnp.float32) * inverse[None, :]
    sign = jnp.where(lane % (HD // 2) < quarter, -1.0, 1.0)
    return jnp.cos(angles), jnp.sin(angles) * sign[None, :]


def row_root(ref, step):
    rows, depth = ref.shape
    total = jnp.zeros((rows, LANES), jnp.float32)
    for k in range(0, depth, step):
        v = ref[:, k : k + step].astype(jnp.float32)
        v = v * v
        for c in range(0, step, LANES):
            total = total + v[:, c : c + LANES]
    return lax.rsqrt(jnp.sum(total, axis=1, keepdims=True) / depth + epsilon)


def context_kernel(context, gain, wk, wv, out):
    depth = wk.shape[0]
    step = min(depth, 512)
    root = row_root(context, step)
    acc = jnp.zeros(out.shape, jnp.float32)
    for k in range(0, depth, step):
        v = context[:, k : k + step].astype(jnp.float32) * root * gain[:, k : k + step]
        wkv = jnp.concatenate([wk[k : k + step, :], wv[k : k + step, :]], axis=1)
        acc = acc + jnp.dot(v.astype(jnp.bfloat16), wkv, preferred_element_type=jnp.float32)
    out[...] = acc.astype(jnp.bfloat16)


def project_kernel(parts, carried, place, *refs):
    x_refs = refs[:parts]
    gain, shift, wq, wk, wv, cosine, sine = refs[parts : parts + 7]
    rest = refs[parts + 7 :]
    if carried:
        q_prev, kv_prev, q_out, kv_out = rest
        q_out[...] = q_prev[...]
        kv_out[...] = kv_prev[...]
    else:
        q_out, kv_out = rest
    depth = wq.shape[0]
    step = min(depth, 512)
    rows = x_refs[0].shape[0]
    query_width = wq.shape[1]
    key_width = wk.shape[1]
    roots = []
    for ref in x_refs:
        roots.append(row_root(ref, step))
    acc_q = jnp.zeros((rows * parts, query_width), jnp.float32)
    acc_kv = jnp.zeros((rows * parts, 2 * key_width), jnp.float32)
    for k in range(0, depth, step):
        pieces = []
        for ref, root in zip(x_refs, roots):
            v = ref[:, k : k + step].astype(jnp.float32) * root
            v = v * gain[:, k : k + step] + shift[:, k : k + step]
            pieces.append(v.astype(jnp.bfloat16))
        normed = jnp.concatenate(pieces, axis=0)
        acc_q = acc_q + jnp.dot(
            normed, wq[k : k + step, :], preferred_element_type=jnp.float32
        )
        wkv = jnp.concatenate([wk[k : k + step, :], wv[k : k + step, :]], axis=1)
        acc_kv = acc_kv + jnp.dot(normed, wkv, preferred_element_type=jnp.float32)
    lane = lax.broadcasted_iota(jnp.int32, (rows, LANES), 1)
    first = lane % (HD // 2) < HD // 4
    for i in range(parts):
        start = pl.multiple_of(place[i], 16)
        cos_rows = cosine[pl.ds(start, rows), :]
        sin_rows = sine[pl.ds(start, rows), :]
        for acc, out, width in (
            (acc_q, q_out, query_width),
            (acc_kv, kv_out, key_width),
        ):
            block = acc[i * rows : (i + 1) * rows]
            for c in range(0, block.shape[1], LANES):
                piece = block[:, c : c + LANES]
                turned = min(max(width - c, 0), LANES)
                if turned:
                    other = jnp.where(
                        first,
                        pltpu.roll(piece, LANES - HD // 4, 1),
                        pltpu.roll(piece, HD // 4, 1),
                    )
                    moved = piece * cos_rows + other * sin_rows
                    piece = moved if turned == LANES else jnp.where(lane < turned, moved, piece)
                out[pl.ds(start, rows), c : c + LANES] = piece.astype(jnp.bfloat16)


def project(blocks, places, gain, shift, wq, wk, wv, tables, carried, out_rows):
    parts = len(blocks)
    depth, query_width = wq.shape
    kv_width = 2 * wk.shape[1]
    rows = blocks[0].shape[0] * parts
    return pl.pallas_call(
        functools.partial(project_kernel, parts, bool(carried)),
        out_shape=(
            jax.ShapeDtypeStruct((out_rows, query_width), jnp.bfloat16),
            jax.ShapeDtypeStruct((out_rows, kv_width), jnp.bfloat16),
        ),
        in_specs=[SMEM] + [VMEM] * (parts + 7 + len(carried)),
        out_specs=(VMEM, VMEM),
        compiler_params=pltpu.CompilerParams(vmem_limit_bytes=24 * 1024 * 1024),
        cost_estimate=cost(
            2 * rows * depth * (query_width + kv_width), 2 * depth * (rows + query_width + kv_width)
        ),
    )(jnp.stack(places), *blocks, gain, shift, wq, wk, wv, *tables, *carried)


def attend_block(q, band, ctx_refs, sink, out, out_row, low, high):
    key_width = ctx_refs[0].shape[1] // 2
    group = HEADS // KV_HEADS
    row = lax.broadcasted_iota(jnp.int32, (WIN, WIN), 0)
    col = lax.broadcasted_iota(jnp.int32, (WIN, WIN), 1)
    before = col >= row
    after = col <= row
    if low is not None:
        before = before & (low != 0)
    if high is not None:
        after = after & (high != 0)
    before = jnp.concatenate([before] * group, axis=0)
    after = jnp.concatenate([after] * group, axis=0)
    contract = (((1,), (1,)), ((), ()))
    for head in range(key_width // HD):
        base = head * group * HD
        query = jnp.concatenate(
            [q[:, base + g * HD : base + (g + 1) * HD] for g in range(group)], axis=0
        )
        query = query * jnp.asarray(HD**-0.5, jnp.bfloat16)
        ks = slice(head * HD, (head + 1) * HD)
        vs = slice(key_width + head * HD, key_width + (head + 1) * HD)
        scores = [
            lax.dot_general(
                query, ref[r : r + WIN, ks], contract, preferred_element_type=jnp.float32
            )
            for ref, r in band
        ] + [
            lax.dot_general(query, ref[:, ks], contract, preferred_element_type=jnp.float32)
            for ref in ctx_refs
        ]
        scores[0] = jnp.where(before, scores[0], neg_large)
        scores[2] = jnp.where(after, scores[2], neg_large)
        sinks = jnp.concatenate(
            [jnp.full((WIN, 1), sink[head * group + g], jnp.float32) for g in range(group)], axis=0
        )
        top = sinks
        for s in scores:
            top = jnp.maximum(top, jnp.max(s, axis=1, keepdims=True))
        values = [ref[r : r + WIN, vs] for ref, r in band] + [ref[:, vs] for ref in ctx_refs]
        gathered = jnp.zeros((group * WIN, 2 * HD), jnp.float32)
        for s, v in zip(scores, values):
            power = jnp.exp(s - top).astype(jnp.bfloat16)
            joined = jnp.concatenate([v, jnp.ones_like(v)], axis=1)
            gathered = gathered + jnp.dot(power, joined, preferred_element_type=jnp.float32)
        total = gathered[:, HD : HD + 1] + jnp.exp(sinks - top)
        gathered = gathered[:, :HD] * (1.0 / total)
        for g in range(group):
            out[out_row : out_row + WIN, base + g * HD : base + (g + 1) * HD] = gathered[
                g * WIN : (g + 1) * WIN
            ].astype(jnp.bfloat16)


def inner_kernel(blocks, sink, q, kv, *refs):
    ctx, out = refs[:-1], refs[-1]
    for n in range(1, blocks - 1):
        band = [(kv, (n + s) * WIN) for s in (-1, 0, 1)]
        attend_block(
            q[n * WIN : (n + 1) * WIN, :], band, ctx, sink, out, (n - 1) * WIN, None, None
        )


def edge_kernel(blocks, inner, ends, sink, q, kv, head, tail, *refs):
    if inner:
        ctx, middle, out = refs[:-2], refs[-2], refs[-1]
        out[WIN : (blocks - 1) * WIN, :] = middle[...]
    else:
        ctx, out = refs[:-1], refs[-1]
    for n in sorted({0, blocks - 1}):
        band = [
            (head, 0) if n == 0 else (kv, (n - 1) * WIN),
            (kv, n * WIN),
            (tail, 0) if n == blocks - 1 else (kv, (n + 1) * WIN),
        ]
        attend_block(
            q[n * WIN : (n + 1) * WIN, :],
            band,
            ctx,
            sink,
            out,
            n * WIN,
            ends[0] if n == 0 else None,
            ends[1] if n == blocks - 1 else None,
        )


def attend_cost(blocks, query_width, ctx):
    keys = 3 * WIN + sum(c.shape[0] for c in ctx)
    return cost(4 * blocks * WIN * keys * query_width * 4, 2**20)


def out_kernel(parts, rows, place, *refs):
    att, weight, outs = refs[:parts], refs[parts], refs[parts + 1 :]
    width = att[0].shape[1]
    for i in range(len(outs)):
        start = pl.multiple_of(place[i], 16)
        total = jnp.zeros((rows, weight.shape[1]), jnp.float32)
        for k in range(parts):
            total = total + jnp.dot(
                att[k][pl.ds(start, rows), :],
                weight[k * width : (k + 1) * width, :],
                preferred_element_type=jnp.float32,
            )
        outs[i][...] = total.astype(jnp.bfloat16)


def out_rows(att, weight, places, rows):
    parts = len(att)
    count = len(places)
    return pl.pallas_call(
        functools.partial(out_kernel, parts, rows),
        out_shape=tuple(
            jax.ShapeDtypeStruct((rows, weight.shape[1]), jnp.bfloat16) for _ in range(count)
        ),
        in_specs=[SMEM] + [VMEM] * (parts + 1),
        out_specs=tuple(VMEM for _ in range(count)),
        compiler_params=pltpu.CompilerParams(vmem_limit_bytes=16 * 1024 * 1024),
        cost_estimate=cost(2 * rows * count * weight.shape[0] * weight.shape[1], 2**22),
    )(jnp.stack(places), *att, weight)


def finish_kernel(place, latent, gate, blend, *refs):
    refs[-1][...] = (
        latent[...].astype(jnp.float32) + gate[...] * blend[...].astype(jnp.float32)
    ).astype(jnp.bfloat16)


def finish(latent, gate, blend, place, mixed):
    rows, width = blend.shape
    there = pl.BlockSpec((rows, width), lambda i, place: (0, place[0]))
    here = pl.BlockSpec((rows, width), lambda i, place: (0, 0))
    line = pl.BlockSpec((1, width), lambda i, place: (0, place[0]))
    return pl.pallas_call(
        finish_kernel,
        out_shape=jax.ShapeDtypeStruct(latent.shape, jnp.bfloat16),
        grid_spec=pltpu.PrefetchScalarGridSpec(
            num_scalar_prefetch=1,
            grid=(1,),
            in_specs=[there, line, here] + [pl.BlockSpec(memory_space=pl.ANY)] * len(mixed),
            out_specs=there,
        ),
        input_output_aliases={4: 0} if mixed else {},
        compiler_params=pltpu.CompilerParams(vmem_limit_bytes=8 * 1024 * 1024),
        cost_estimate=cost(2**20, 2**20),
    )(place[None], latent, gate, blend, *mixed)


def local(
    latent,
    context,
    conditioning,
    norm_gain,
    shift_weight,
    scale_weight,
    gate_weight,
    query_weight,
    key_weight,
    value_weight,
    out_weight,
    sink_logit,
):
    count = lax.axis_size("tp")
    chips = count // CORES
    me = lax.axis_index("tp")
    chip, core = me // CORES, me % CORES
    ring = lax.axis_size("sp")
    rank = lax.axis_index("sp")
    rows, depth = latent.shape
    row_count = rows * count
    cuts = 2
    piece = rows // cuts

    def index(step, flip):
        return ((chip + step) % chips) * CORES + (core ^ flip)

    near = [latent, from_partner(latent, count)]
    near_place = [index(0, 0) * rows, index(0, 1) * rows]
    far, far_place = [], []
    for step in range(1, chips):
        for cut in range(cuts):
            got = from_chip(latent[cut * piece : (cut + 1) * piece], count, step)
            far += [got, from_partner(got, count)]
            far_place += [index(step, flip) * rows + cut * piece for flip in (0, 1)]

    lifted = jax.nn.silu(conditioning.astype(jnp.float32)).astype(jnp.bfloat16)[None, :]
    partial = jnp.concatenate(
        [
            jnp.dot(lifted, w, preferred_element_type=jnp.float32)
            for w in (shift_weight, scale_weight, gate_weight)
        ],
        axis=0,
    )
    partial, context, rank = lax.optimization_barrier((partial, context, rank))
    shares = from_ring(partial, ring)
    summed = functools.reduce(jnp.add, shares)
    sums = [(summed, index(0, 0)), (from_partner(summed, count), index(0, 1))]
    for step in range(1, chips):
        for flip in range(CORES):
            sums.append((send_rows(summed, count, -step, flip), index(step, flip)))
    line = jax.ShapeDtypeStruct((1, depth), jnp.float32)
    gain_vec, shift_vec, gate_vec = pl.pallas_call(
        modulation_kernel,
        out_shape=(line, line, line),
        in_specs=[SMEM] + [VMEM] * (1 + count),
        out_specs=(VMEM, VMEM, VMEM),
        compiler_params=pltpu.CompilerParams(vmem_limit_bytes=8 * 1024 * 1024),
        cost_estimate=cost(2**16, 2**16),
    )(
        jnp.stack([at * summed.shape[1] for _, at in sums]),
        norm_gain[None, :],
        *[block for block, _ in sums],
    )

    own = pl.pallas_call(
        context_kernel,
        out_shape=jax.ShapeDtypeStruct((context.shape[0], 2 * key_weight.shape[1]), jnp.bfloat16),
        in_specs=[VMEM] * 4,
        out_specs=VMEM,
        compiler_params=pltpu.CompilerParams(vmem_limit_bytes=16 * 1024 * 1024),
        cost_estimate=cost(4 * context.shape[0] * depth * key_weight.shape[1], 2**22),
    )(context, norm_gain[None, :], key_weight, value_weight)
    if ring <= 8:
        ctx = from_ring(own, ring)
    else:
        ctx = [lax.all_gather(own, "sp", axis=0, tiled=True)]

    row_offset = rank * row_count
    tables = turn_tables(row_offset + jnp.arange(row_count, dtype=jnp.int32))
    args = (gain_vec, shift_vec, query_weight, key_weight, value_weight, tables)
    queries, key_value = project(near, near_place, *args, (), row_count)
    if far:
        queries, key_value = project(
            far, far_place, *args, (queries, key_value), row_count
        )

    head = lax.ppermute(
        key_value[row_count - WIN :], "sp", [(i, i + 1) for i in range(ring - 1)]
    )
    tail = lax.ppermute(key_value[:WIN], "sp", [(i + 1, i) for i in range(ring - 1)])
    blocks = row_count // WIN
    query_width = query_weight.shape[1]
    limit = pltpu.CompilerParams(vmem_limit_bytes=16 * 1024 * 1024)
    middle = ()
    if blocks > 2:
        middle = (
            pl.pallas_call(
                functools.partial(inner_kernel, blocks),
                out_shape=jax.ShapeDtypeStruct(((blocks - 2) * WIN, query_width), jnp.bfloat16),
                in_specs=[SMEM] + [VMEM] * (2 + len(ctx)),
                out_specs=VMEM,
                compiler_params=limit,
                cost_estimate=attend_cost(blocks - 2, query_width, ctx),
            )(sink_logit, queries, key_value, *ctx),
        )
    ends = jnp.stack([(rank > 0).astype(jnp.int32), (rank < ring - 1).astype(jnp.int32)])
    attended = pl.pallas_call(
        functools.partial(edge_kernel, blocks, bool(middle)),
        out_shape=jax.ShapeDtypeStruct((row_count, query_width), jnp.bfloat16),
        in_specs=[SMEM, SMEM] + [VMEM] * (4 + len(ctx) + len(middle)),
        out_specs=VMEM,
        compiler_params=limit,
        cost_estimate=attend_cost(2, query_width, ctx),
    )(ends, sink_logit, queries, key_value, head, tail, *ctx, *middle)

    att, order = [], []
    for step in range(chips):
        got = attended if step == 0 else from_chip(attended, count, step)
        att += [got, from_partner(got, count)]
        order += [index(step, 0), index(step, 1)]
    weight = jnp.concatenate(
        [
            lax.dynamic_slice_in_dim(out_weight, source * query_width, query_width, 0)
            for source in order
        ],
        axis=0,
    )

    steps = [(step, flip) for step in range(1, chips) for flip in range(CORES)]
    received, places = [], []
    if steps:
        sent = out_rows(att, weight, [index(s, f) * rows for s, f in steps], rows)
        for (s, f), block in zip(steps, sent):
            received.append(send_rows(block, count, s, f))
            places.append((((chip - s) % chips) * CORES + (core ^ f)) )
    mine, other = out_rows(att, weight, [index(0, 0) * rows, index(0, 1) * rows], rows)
    near_blends = [(mine, index(0, 0)), (from_partner(other, count), index(0, 1))]
    mixed = ()
    for block, place in near_blends + list(zip(received, places)):
        mixed = (finish(latent, gate_vec, block, place, mixed),)
    return mixed[0]


def solution(mesh):
    in_specs = (
        P(("grp", "sp", "tp"), None),
        P(("grp", "sp"), None),
        P(("grp", "sp")),
        P(),
        P("sp", "tp"),
        P("sp", "tp"),
        P("sp", "tp"),
        P(None, "tp"),
        P(None, "tp"),
        P(None, "tp"),
        P(None, "tp"),
        P("tp"),
    )
    out_specs = P(("grp", "sp", "tp"), None)

    return jax.shard_map(local, mesh=mesh, in_specs=in_specs, out_specs=out_specs, check_vma=False)
```
